32 devices in a mesh: fs: 16 (over z, y, x), tp: 2 (over core).
Axes of the slice: x: 2, y: 2, z: 4, core: 2. Of those that a mesh axis runs over, the one named last changes fastest.
Arguments:
- block_input: bfloat16 [16384, 2048], P('fs'), may hold values from -6 to 6
- value_cotangent: bfloat16 [16384, 1024], P('fs', 'tp'), may hold values from -6 to 6
- mixed_output: bfloat16 [16384, 1024], P('fs', 'tp'), may hold values from -6 to 6
- output_cotangent: bfloat16 [16384, 2048], P('fs'), may hold values from -6 to 6
- value_weight: float32 [2048, 1024], P('fs', 'tp'), may hold values from -0.125 to 0.125
- output_weight: float32 [1024, 2048], P('tp', 'fs'), may hold values from -0.1875 to 0.1875
- value_basis: bfloat16 [2048, 384], P('fs'), may hold values from -0.125 to 0.125
- output_basis: bfloat16 [2048, 384], P('fs'), may hold values from -0.125 to 0.125
- value_mean: float32 [384, 1024], P(None, 'tp'), may hold values from -4 to 4
- value_square: float32 [384, 1024], P(None, 'tp'), may hold values from 0.3 to 2
- output_mean: float32 [1024, 384], P('tp'), may hold values from -4 to 4
- output_square: float32 [1024, 384], P('tp'), may hold values from 0.3 to 2
Outputs:
- value_next: float32 [2048, 1024], P('fs', 'tp')
- value_copy: bfloat16 [2048, 1024], P(None, 'tp')
- value_step: float32 [2048, 1024], P('fs', 'tp')
- value_mean_next: float32 [384, 1024], P(None, 'tp')
- value_square_next: float32 [384, 1024], P(None, 'tp')
- output_next: float32 [1024, 2048], P('tp', 'fs')
- output_copy: bfloat16 [1024, 2048], P('tp')
- output_step: float32 [1024, 2048], P('tp', 'fs')
- output_mean_next: float32 [1024, 384], P('tp')
- output_square_next: float32 [1024, 384], P('tp')
The draws below stay inside these ranges and needn't reach their ends.
All inputs are finite; a program needn't handle non-finite values.
Results may differ from the reference program's by a relative error of at most 0.002.
Values may be sent and summed in bfloat16 or wider, within the bound.
A program may use at most 64 MiB of HBM per device.

```python
import math
import jax
import jax.numpy as jnp
from jax import lax

D = 2048
E = 1024
R = 384
TOKENS = 16384


def block_scale(own_key, dims, shards, smallest, high):
    loudness = 1.0
    for axis_at, parts in shards:
        draws = jax.random.uniform(jax.random.fold_in(jax.random.fold_in(own_key, 6), axis_at), (parts,), jnp.float32, smallest / len(shards), high / len(shards))
        loudness = loudness * jnp.repeat(jnp.exp(draws), dims[axis_at] // parts).reshape((-1,) + (1,) * (len(dims) - 1 - axis_at))
    return loudness


def normal_values(own_key, dims, spread, limit, pieces=(), kind=jnp.bfloat16):
    drawn = spread * jax.random.normal(own_key, dims, jnp.float32)
    if pieces:
        drawn = drawn * block_scale(own_key, dims, pieces, -0.22, 0.18)
    return jnp.clip(drawn, -limit, limit).astype(kind)


def setup_inputs(seed: int = 0) -> dict:
    keys = jax.random.split(jax.random.key(seed), 13)
    return {
        "block_input": normal_values(keys[0], (TOKENS, D), 1.0, 6.0, ((0, 16),)),
        "value_cotangent": normal_values(keys[1], (TOKENS, E), 1.0, 6.0, ((0, 16), (1, 2))),
        "mixed_output": normal_values(keys[2], (TOKENS, E), 1.0, 6.0, ((0, 16), (1, 2))),
        "output_cotangent": normal_values(keys[3], (TOKENS, D), 1.0, 6.0, ((0, 16),)),
        "value_weight": normal_values(keys[4], (D, E), D ** -0.5, 0.125, ((0, 16), (1, 2)), jnp.float32),
        "output_weight": normal_values(keys[5], (E, D), E ** -0.5, 0.1875, ((0, 2), (1, 16)), jnp.float32),
        "value_basis": normal_values(keys[6], (D, R), D ** -0.5, 0.125, ((0, 16),)),
        "output_basis": normal_values(keys[7], (D, R), D ** -0.5, 0.125, ((0, 16),)),
        "value_mean": normal_values(keys[8], (R, E), 0.7, 4.0, ((1, 2),), jnp.float32),
        "value_square": jnp.clip(jnp.exp(math.log(2.0) - 1.89712 * jax.random.uniform(keys[9], (R, E), jnp.float32) ** block_scale(keys[9], (R, E), ((1, 2),), -0.2, 0.2)), 0.3, 2.0),
        "output_mean": normal_values(keys[10], (E, R), 0.7, 4.0, ((0, 2),), jnp.float32),
        "output_square": jnp.clip(jnp.exp(math.log(2.0) - 1.89712 * jax.random.uniform(keys[11], (E, R), jnp.float32) ** block_scale(keys[11], (E, R), ((0, 2),), -0.2, 0.2)), 0.3, 2.0),
    }


def reference(block_input, value_cotangent, mixed_output, output_cotangent, value_weight, output_weight, value_basis, output_basis, value_mean, value_square, output_mean, output_square):
    highest = lax.Precision.HIGHEST
    scaling = 1.0 / math.sqrt(TOKENS)
    value_grad = jnp.dot(block_input.T, value_cotangent, preferred_element_type=jnp.float32)
    output_grad = jnp.dot(mixed_output.T, output_cotangent, preferred_element_type=jnp.float32)
    value_base = value_basis.astype(jnp.float32)
    output_base = output_basis.astype(jnp.float32)
    value_low = jnp.dot(value_base.T, value_grad, precision=highest) * scaling
    output_low = jnp.dot(output_grad, output_base, precision=highest) * scaling
    total_squares = jnp.sum(value_low * value_low) + jnp.sum(output_low * output_low)
    clip_scale = 1.0 / jnp.sqrt(1.0 + total_squares / (2.0 * R * E))
    value_scaled = clip_scale * value_low
    output_scaled = clip_scale * output_low
    value_mean_next = 0.8 * value_mean + 0.2 * value_scaled
    output_mean_next = 0.8 * output_mean + 0.2 * output_scaled
    value_square_next = 0.9 * value_square + 0.1 * value_scaled * value_scaled
    output_square_next = 0.9 * output_square + 0.1 * output_scaled * output_scaled
    value_norm = value_mean_next / jnp.sqrt(value_square_next + 0.1)
    output_norm = output_mean_next / jnp.sqrt(output_square_next + 0.1)
    value_step = jnp.dot(value_base, value_norm, precision=highest)
    output_step = jnp.dot(output_norm, output_base.T, precision=highest)
    value_next = value_weight - 0.02 * value_step
    output_next = output_weight - 0.02 * output_step
    return (value_next, value_next.astype(jnp.bfloat16), value_step, value_mean_next, value_square_next, output_next, output_next.astype(jnp.bfloat16), output_step, output_mean_next, output_square_next)
```

```python
import functools
import math

import jax
import jax.numpy as jnp
from jax import lax
from jax.experimental import pallas as pl
from jax.experimental.pallas import tpu as pltpu
from jax.sharding import PartitionSpec as P

MESH = pl.DeviceIdType.MESH
VALUE_RATE = 125.0 / 0.125
OUTPUT_RATE = 125.0 / 0.1875
LOW_RATE = 124.0
BLOCK_LANES = 256
TOKEN_TILE = 256
FIRST = (((0,), (0,)), ((), ()))
LAST = (((1,), (1,)), ((), ()))


def split_fs(n):
    inner = 2 if n % 2 == 0 else 1
    middle = 2 if n % (2 * inner) == 0 else 1
    return n // (inner * middle), middle, inner


class Place:
    def __init__(self, n):
        self.sizes = split_fs(n)
        self.me = lax.axis_index("fs")
        self.core = lax.axis_index("tp")
        self.par = lax.rem(self.core, 2)
        self.partner = self.core + 1 - 2 * self.par
        a, b, c = self.sizes
        self.z = self.me // (b * c)
        self.y = lax.rem(self.me // c, b)
        self.x = lax.rem(self.me, c)
        self.planes = [self.near(i) for i in range(a)]

    def near(self, i):
        a = self.sizes[0]
        low = jnp.minimum(self.z, a - 1 - self.z)
        side = self.z - (i + 1) // 2 if i % 2 else self.z + i // 2
        return jnp.where(2 * low >= i, side, jnp.where(self.z <= a - 1 - self.z, i, a - 1 - i))

    def on(self, z, ds, dt, par=None):
        a, b, c = self.sizes
        par = self.par if par is None else par
        y = lax.rem(self.y + ds * (1 - par) + dt * par, b)
        x = lax.rem(self.x + ds * par + dt * (1 - par), c)
        return (z * b + y) * c + x

    def at(self, dz, ds, dt):
        return self.on(lax.rem(self.z + dz, self.sizes[0]), ds, dt)


class Gather:
    def __init__(self, place, slot, send, recv, line=False, plane_first=False, seen=None):
        self.p, self.slot, self.send, self.recv = place, slot, send, recv
        self.line, self.plane_first, self.seen = line, plane_first, seen or (lambda *k: None)
        self.a = place.sizes[0]
        self.started = []

    def copy(self, src, ds, to, kind, sid, rid):
        ref = self.slot(self.p.on(src, ds, 0))
        return pltpu.make_async_remote_copy(
            src_ref=ref, dst_ref=ref, send_sem=self.send.at[kind, sid], recv_sem=self.recv.at[rid],
            device_id={"fs": to}, device_id_type=MESH)

    def go(self, src, ds, to, kind, sid, rid, when=None):
        def make():
            return self.copy(src, ds, to, kind, sid, rid)

        self.started.append((make, when))
        if when is None:
            make().start()
        else:
            @pl.when(when)
            def _():
                make().start()

    def came(self, src, ds, dt):
        ref = self.slot(self.p.on(src, ds, dt))
        pltpu.make_async_remote_copy(
            src_ref=ref, dst_ref=ref, send_sem=self.send.at[0, 0], recv_sem=self.recv.at[(src * 2 + ds) * 2 + dt],
            device_id={"fs": self.p.me}, device_id_type=MESH).wait_recv()

    def to_s(self, src):
        self.go(src, 0, self.p.on(self.p.z, 1, 0), 2, src * 2, (src * 2 + 1) * 2)

    def to_t(self, src, ds):
        self.go(src, ds, self.p.on(self.p.z, 0, 1), 3, src * 2 + ds, (src * 2 + ds) * 2 + 1)

    def begin_z(self, ds=0):
        z, rid = self.p.z, (self.p.z * 2 + ds) * 2
        if self.line:
            self.go(z, ds, self.p.on(z + 1, 0, 0), 0, z * 2 + ds, rid, z < self.a - 1)
            self.go(z, ds, self.p.on(z - 1, 0, 0), 1, z * 2 + ds, rid, z > 0)
        else:
            for dz in range(1, self.a):
                self.go(z, ds, self.p.at(dz, 0, 0), 0, dz * 2 + ds, rid)

    def begin_st(self):
        self.to_s(self.p.z)
        self.to_t(self.p.z, 0)
        self.seen(self.p.z, 0, 0)

    def begin(self):
        self.begin_z()
        self.begin_st()

    def near_s(self):
        self.came(self.p.z, 1, 0)
        self.begin_z(1)
        self.to_t(self.p.z, 1)
        self.seen(self.p.z, 1, 0)

    def z(self, k, ds=0):
        if k >= self.a:
            return
        src, z = self.p.planes[k], self.p.z
        self.came(src, ds, 0)
        if self.line:
            up = src < z
            to = jnp.clip(jnp.where(up, z + 1, z - 1), 0, self.a - 1)
            inside = jnp.where(up, z + 1, self.a - z) < self.a
            self.go(src, ds, self.p.on(to, 0, 0), 0, src * 2 + ds, (src * 2 + ds) * 2, inside)
        if not self.plane_first:
            self.to_s(src)
        self.to_t(src, ds)
        self.seen(src, ds, 0)

    def s(self, k):
        if k < self.a:
            src = self.p.planes[k]
            self.came(src, 1, 0)
            self.to_t(src, 1)
            self.seen(src, 1, 0)

    def t(self, k):
        if k < self.a:
            for ds in range(2):
                self.came(self.p.planes[k], ds, 1)
                self.seen(self.p.planes[k], ds, 1)

    def last(self):
        for k in range(self.a):
            self.t(k)

    def finish(self):
        for make, when in self.started:
            if when is None:
                make().wait_send()
            else:
                @pl.when(when)
                def _():
                    make().wait_send()


class Bases(Gather):
    def __init__(self, place, ref, send, recv, c_send, c_recv):
        half = ref.shape[1] // 2
        rows = [pl.ds(pl.multiple_of(side * half, half), half) for side in (place.par, 1 - place.par)]
        super().__init__(place, lambda i: ref.at[i, rows[0]], send, recv, line=False, seen=self.cross)
        self.other = lambda i: ref.at[i, rows[1]]
        self.c_send, self.c_recv = c_send, c_recv
        self.crossed = []

    def over(self, ref, k):
        return pltpu.make_async_remote_copy(
            src_ref=ref, dst_ref=ref, send_sem=self.c_send.at[k], recv_sem=self.c_recv.at[k],
            device_id={"tp": self.p.partner}, device_id_type=MESH)

    def cross(self, src, ds, dt):
        c = self.over(self.slot(self.p.on(src, ds, dt)), (src * 2 + ds) * 2 + dt)
        c.start()
        self.crossed.append(c)

    def whole(self):
        for src in range(self.a):
            for ds in range(2):
                for dt in range(2):
                    self.over(self.other(self.p.on(src, ds, dt, 1 - self.p.par)), (src * 2 + ds) * 2 + dt).wait_recv()

    def finish(self):
        super().finish()
        for c in self.crossed:
            c.wait_send()


def halves(value):
    high = value.astype(jnp.bfloat16)
    return high, (value - high.astype(jnp.float32)).astype(jnp.bfloat16)


def one(reduce, value):
    return reduce(reduce(value, axis=1, keepdims=True), axis=0, keepdims=True)


def bound(values):
    top = jnp.maximum(one(jnp.max, jnp.abs(values)) * 1.01, 1e-30)
    return top.astype(jnp.bfloat16).astype(jnp.float32)


def encode(values, entries, rows):
    row = lax.broadcasted_iota(jnp.int32, (rows - values.shape[0], values.shape[1]), 0)
    extra = jnp.zeros(row.shape, jnp.float32)
    for k, entry in enumerate(entries):
        extra = jnp.where(row == k, entry.astype(jnp.float32), extra)
    return jnp.concatenate([jnp.exp2((LOW_RATE / entries[0]) * values), extra], axis=0).astype(jnp.bfloat16)


def decode(code, high):
    top = code[high:high + 1].astype(jnp.float32)
    return top * (1.0 / LOW_RATE) * jnp.log2(code[:high].astype(jnp.float32)), top


class Scatter:
    def __init__(self, place, part, code, got, send, recv):
        self.p, self.part, self.code, self.got, self.send, self.recv = place, part, code, got, send, recv
        self.a = place.sizes[0]
        self.order = list(range(1, self.a)) + [0]
        self.started = []

    def copy(self, block, to, slot):
        return pltpu.make_async_remote_copy(
            src_ref=self.code.at[block], dst_ref=self.got.at[slot],
            send_sem=self.send.at[slot], recv_sem=self.recv.at[slot],
            device_id={"fs": to}, device_id_type=MESH)

    def hand(self, block, to, slot, top):
        self.code[block] = encode(self.part[block], (top,), self.code.shape[1])
        c = self.copy(block, to, slot)
        c.start()
        self.started.append(c)

    def take(self, block, slot):
        self.copy(block, self.p.me, slot).wait_recv()
        value, top = decode(self.got[slot], self.part.shape[1])
        self.part[block] += value
        return top.astype(jnp.bfloat16).astype(jnp.float32)

    def grown(self, top):
        return top.astype(jnp.bfloat16).astype(jnp.float32)

    def give_t(self):
        n, high, width = self.part.shape
        self.top = jnp.broadcast_to(bound(self.part[...].reshape(n * high, width)), (1, width))
        for dz in self.order:
            for ds in (1, 0):
                self.hand(self.p.at(dz, ds, 1), self.p.on(self.p.z, 0, 1), dz * 2 + ds, self.top)

    def turn_s(self, i):
        if i < self.a:
            dz = self.order[i]
            top = self.take(self.p.at(dz, 1, 0), dz * 2 + 1)
            if i == 0:
                self.top = self.grown(self.top + top)
            self.hand(self.p.at(dz, 1, 0), self.p.on(self.p.z, 1, 0), 2 * self.a + dz, self.top)
            self.take(self.p.at(dz, 0, 0), dz * 2)

    def turn_z(self, i):
        if i < self.a:
            dz = self.order[i]
            top = self.take(self.p.at(dz, 0, 0), 2 * self.a + dz)
            if i == 0:
                self.top = self.grown(self.top + top)
            if dz:
                self.hand(self.p.at(dz, 0, 0), self.p.at(dz, 0, 0), 3 * self.a + dz, self.top)

    def end(self):
        for dz in range(1, self.a):
            self.take(self.p.me, 3 * self.a + dz)

    def finish(self):
        for c in self.started:
            c.wait_send()


def twice(basis):
    return jnp.concatenate([basis, basis], axis=1)


def exchange(n, scaling, entries, x_hbm, v_hbm, m_hbm, o_hbm, vb_hbm, ob_hbm, vw_hbm, ow_hbm, vm_hbm, vs_hbm, om_hbm, os_hbm,
             v_next, v_copy, v_step, vm_next, vs_next, o_next, o_copy, o_step, om_next, os_next,
             bases, wv, wo, low, sums, vw, ow, x_ref, v_ref, m_ref, o_ref, vm, vs, om, os, part, code, got, small, norms_v, norms_o,
             load_sem, own_sem, b_send, b_recv, c_send, c_recv, w_send, w_recv, l_send, l_recv, r_send, r_recv, q_send, q_recv):
    p = Place(n)
    a, b, c = p.sizes
    par, me = p.par, p.me
    half = bases.shape[2] // 2
    mine = pl.ds(pl.multiple_of(par * half, half), half)
    own = [pltpu.make_async_copy(s.at[mine], bases.at[i, me, mine], own_sem.at[i]) for i, s in enumerate((vb_hbm, ob_hbm))]
    loads = [pltpu.make_async_copy(s, d, load_sem.at[i]) for i, (s, d) in enumerate(
        ((vw_hbm, vw), (ow_hbm, ow), (o_hbm, o_ref), (m_hbm, m_ref), (x_hbm, x_ref), (v_hbm, v_ref),
         (vm_hbm, vm), (vs_hbm, vs), (om_hbm, om), (os_hbm, os)))]
    for c_ in own + loads:
        c_.start()
    barrier = pltpu.get_barrier_semaphore()
    near = [p.at(dz, 0, 0) for dz in range(1, a)] + [p.on(p.z, 1, 0), p.on(p.z, 0, 1)]
    for to in near:
        pl.semaphore_signal(barrier, inc=1, device_id={"fs": to}, device_id_type=MESH)
    cores = lax.axis_size("tp")
    siblings = [lax.rem(p.core + d, cores) for d in range(1, cores)]
    for to in siblings:
        pl.semaphore_signal(barrier, inc=1, device_id={"tp": to}, device_id_type=MESH)
    pl.semaphore_wait(barrier, len(near) + len(siblings))
    for c_ in own:
        c_.wait()

    bv, bo = (Bases(p, bases.at[j], b_send.at[j], b_recv.at[j], c_send.at[j], c_recv.at[j]) for j in range(2))
    w0, w1 = (Gather(p, lambda i, ref=ref: ref.at[i], w_send.at[j], w_recv.at[j], line=True, plane_first=first)
              for j, (ref, first) in enumerate(((wv, False), (wo, True))))
    rv, ro = (Scatter(p, part.at[j], code.at[j], got.at[j], r_send.at[j], r_recv.at[j]) for j in range(2))
    lv, lo = (Gather(p, lambda i, j=j: low.at[j, i], l_send.at[j], l_recv.at[j]) for j in range(2))

    depth, rank = bases.shape[2], bases.shape[3]
    high, width = part.shape[2], part.shape[3]
    tokens = x_ref.shape[0]
    tile = math.gcd(tokens, TOKEN_TILE)
    steps = tokens // tile
    far = range(3, a)

    def product(j, start, stop):
        wide, thin = ((x_ref, v_ref), (o_ref, m_ref))[j]

        @pl.loop(start, stop)
        def _(step):
            rows = pl.ds(pl.multiple_of(step * tile, tile), tile)
            thick = jnp.dot(wide[rows, :], bases[j].reshape(n * depth, rank), preferred_element_type=jnp.float32)
            both = jnp.concatenate(halves(thick), axis=0)
            cot = jnp.concatenate([thin[rows, :]] * 2, axis=0)
            part[j] += lax.dot_general(both, cot, FIRST, preferred_element_type=jnp.float32).reshape(n, high, width)

    def pack(j):
        value = part[j, me] * scaling
        low[j, me] = encode(value, (bound(value),) + halves(one(jnp.sum, value * value)), low.shape[2])

    def unpack(j):
        total = jnp.zeros((1, 128), jnp.float32)
        for i in range(n):
            block = low[j, i]
            small[j, i * high:(i + 1) * high] = decode(block, high)[0]
            tail = block[high:].astype(jnp.float32)
            total += tail[1:2, :128] + tail[2:3, :128]
        return total

    def share(total):
        sums[p.core] = jnp.broadcast_to(total, sums.shape[1:])
        out = []
        for d, to in enumerate(siblings):
            out.append(pltpu.make_async_remote_copy(
                src_ref=sums.at[p.core], dst_ref=sums.at[p.core], send_sem=q_send.at[d], recv_sem=q_recv.at[d],
                device_id={"tp": to}, device_id_type=MESH))
            out[-1].start()
        return out

    def shared():
        for d in range(cores - 1):
            ref = sums.at[lax.rem(p.core - d - 1 + cores, cores)]
            pltpu.make_async_remote_copy(
                src_ref=ref, dst_ref=ref, send_sem=q_send.at[d], recv_sem=q_recv.at[d],
                device_id={"tp": p.partner}, device_id_type=MESH).wait_recv()

    def update():
        total = sums[0, :1, :1]
        for i in range(1, cores):
            total += sums[i, :1, :1]
        clip = 1.0 / jnp.sqrt(1.0 + total / entries)
        for scaled, mean, square, mean_next, square_next, norms, at in (
            (clip * small[0], vm, vs, vm_next, vs_next, norms_v, lambda k: (slice(k * rank, (k + 1) * rank), slice(None))),
            (clip * small[1].T, om, os, om_next, os_next, norms_o, lambda k: (slice(None), slice(k * rank, (k + 1) * rank))),
        ):
            mean_new = 0.8 * mean[...] + 0.2 * scaled
            square_new = 0.9 * square[...] + 0.1 * scaled * scaled
            mean_next[...] = mean_new
            square_next[...] = square_new
            for k, part_ in enumerate(halves(mean_new / jnp.sqrt(square_new + 0.1))):
                norms[at(k)] = part_

    def value_steps(basis):
        return jnp.dot(twice(basis), norms_v[...], preferred_element_type=jnp.float32)

    def output_steps(basis):
        return lax.dot_general(norms_o[...], twice(basis), LAST, preferred_element_type=jnp.float32)

    def own_steps():
        v_step[...] = value_steps(bases[0, me])
        v_next[...] = vw[...] - 0.02 * v_step[...]
        o_step[...] = output_steps(bases[1, me])
        o_next[...] = ow[...] - 0.02 * o_step[...]

    def copies(k):
        if k >= a:
            return
        plane = b * c
        count = math.gcd(plane, max(1, BLOCK_LANES // depth))
        span = count * depth

        @pl.loop(0, plane // count)
        def _(i):
            shard = p.planes[k] * plane + i * count
            shards = pl.ds(shard, count)
            to = pl.ds(pl.multiple_of(shard * depth, span), span)
            old = jnp.log2(wv[shards].astype(jnp.float32)).reshape(span, width) * (1.0 / VALUE_RATE)
            v_copy[to, :] = (old - 0.02 * value_steps(bases[0, shards].reshape(span, rank))).astype(v_copy.dtype)
            old = jnp.concatenate([wo[shard + q].astype(jnp.float32) for q in range(count)], axis=1)
            old = jnp.log2(old) * (1.0 / OUTPUT_RATE)
            o_copy[:, to] = (old - 0.02 * output_steps(bases[1, shards].reshape(span, rank))).astype(o_copy.dtype)

    bo.begin_z()
    bo.begin_st()
    bv.begin_z()
    bv.begin_st()
    part[...] = jnp.zeros_like(part)
    for c_ in loads[:2]:
        c_.wait()
    wv[me] = jnp.exp2(VALUE_RATE * vw[...]).astype(wv.dtype)
    wo[me] = jnp.exp2(OUTPUT_RATE * ow[...]).astype(wo.dtype)
    bo.z(1)
    bo.z(2)
    for k in far:
        bo.z(k)
    bo.s(0)
    bo.s(1)
    bo.s(2)
    for k in far:
        bo.s(k)
    bv.z(1)
    bv.z(2)
    for k in far:
        bv.z(k)
    bv.s(0)
    bv.s(1)
    bv.s(2)
    for k in far:
        bv.s(k)
    w0.begin_z()
    w0.begin_st()
    w1.begin_z()
    w1.begin_st()
    bo.last()
    bo.whole()
    for c_ in loads[2:4]:
        c_.wait()
    product(1, 0, steps // 2)
    product(1, steps // 2, steps)
    ro.give_t()
    bv.last()
    bv.whole()
    for c_ in loads[4:6]:
        c_.wait()
    product(0, 0, steps // 2)
    ro.turn_s(0)
    ro.turn_s(1)
    ro.turn_s(2)
    for k in far:
        ro.turn_s(k)
    product(0, steps // 2, steps)
    rv.give_t()
    w0.z(1)
    w0.z(2)
    for k in far:
        w0.z(k)
    w1.near_s()
    w1.z(1)
    w1.z(2)
    ro.turn_z(0)
    ro.turn_z(1)
    ro.turn_z(2)
    for k in far:
        ro.turn_z(k)
    rv.turn_s(0)
    rv.turn_s(1)
    rv.turn_s(2)
    for k in far:
        rv.turn_s(k)
    ro.end()
    pack(1)
    lo.begin_z()
    lo.begin_st()
    rv.turn_z(0)
    rv.turn_z(1)
    rv.turn_z(2)
    for k in far:
        rv.turn_z(k)
    lo.z(1)
    lo.z(2)
    for k in far:
        lo.z(k)
    rv.end()
    pack(0)
    lv.begin_z()
    lv.begin_st()
    w0.s(0)
    w0.s(1)
    w0.s(2)
    for k in far:
        w0.s(k)
    for k in far:
        w1.z(k)
    w1.z(1, 1)
    w1.z(2, 1)
    for k in far:
        w1.z(k, 1)
    lo.s(0)
    lo.s(1)
    lo.s(2)
    for k in far:
        lo.s(k)
    lv.z(1)
    lv.z(2)
    for k in far:
        lv.z(k)
    lo.last()
    total = unpack(1)
    lv.s(0)
    lv.s(1)
    lv.s(2)
    for k in far:
        lv.s(k)
    lv.last()
    total_v = unpack(0)
    sent = share(total + total_v)
    shared()
    for c_ in loads[6:]:
        c_.wait()
    update()
    own_steps()
    w0.t(0)
    w1.t(0)
    copies(0)
    w0.t(1)
    w1.t(1)
    copies(1)
    w0.t(2)
    w1.t(2)
    copies(2)
    for k in far:
        w0.t(k)
    for k in far:
        w1.t(k)
    for k in far:
        copies(k)
    for done in sent:
        done.wait_send()
    for g in (bo, bv, w0, w1, ro, rv, lo, lv):
        g.finish()


def place_out(*refs):
    count = (len(refs) - 1) // 2
    moves = [pltpu.make_async_copy(refs[i], refs[count + i], refs[-1].at[i]) for i in range(count)]
    for move in moves:
        move.start()
    for move in moves:
        move.wait()


def on_device(
    block_input,
    value_cotangent,
    mixed_output,
    output_cotangent,
    value_weight,
    output_weight,
    value_basis,
    output_basis,
    value_mean,
    value_square,
    output_mean,
    output_square,
):
    n, cores = lax.axis_size("fs"), lax.axis_size("tp")
    depth, rank = value_basis.shape
    tokens, width = value_cotangent.shape
    wide = block_input.shape[1]
    a = split_fs(n)[0]
    scaling = 1.0 / math.sqrt(tokens * n)
    entries = 2.0 * rank * width * cores
    f32, b16 = jnp.float32, jnp.bfloat16
    high = rank // n
    rows = (high + 18) // 16 * 16
    hbm = pl.BlockSpec(memory_space=pltpu.HBM)
    vmem = pl.BlockSpec(memory_space=pltpu.VMEM)
    dma = pltpu.SemaphoreType.DMA
    v_row, v_all, v_small = ((depth, width), f32), ((n * depth, width), b16), ((rank, width), f32)
    o_row, o_all, o_small = ((width, depth), f32), ((width, n * depth), b16), ((width, rank), f32)
    outs = (v_row, v_all, v_row, v_small, v_small, o_row, o_all, o_row, o_small, o_small)
    ready = pl.pallas_call(
        functools.partial(exchange, n, scaling, entries),
        out_shape=[pltpu.VMEM(*out) for out in outs],
        in_specs=[hbm] * 12,
        out_specs=[vmem] * len(outs),
        scratch_shapes=[
            pltpu.VMEM((2, n, depth, rank), b16), pltpu.VMEM((n, depth, width), b16), pltpu.VMEM((n, width, depth), b16),
            pltpu.VMEM((2, n, rows, width), b16), pltpu.VMEM((cores, 8, 128), f32),
            pltpu.VMEM((depth, width), f32), pltpu.VMEM((width, depth), f32),
            pltpu.VMEM((tokens, wide), b16), pltpu.VMEM((tokens, width), b16),
            pltpu.VMEM((tokens, width), b16), pltpu.VMEM((tokens, wide), b16),
            pltpu.VMEM((rank, width), f32), pltpu.VMEM((rank, width), f32),
            pltpu.VMEM((width, rank), f32), pltpu.VMEM((width, rank), f32),
            pltpu.VMEM((2, n, high, width), f32), pltpu.VMEM((2, n, rows, width), b16), pltpu.VMEM((2, 4 * a, rows, width), b16),
            pltpu.VMEM((2, rank, width), f32), pltpu.VMEM((2 * rank, width), b16), pltpu.VMEM((width, 2 * rank), b16),
            dma((10,)), dma((2,)),
            dma((2, 4, 2 * a)), dma((2, 4 * a)), dma((2, 4 * a)), dma((2, 4 * a)),
            dma((2, 4, 2 * a)), dma((2, 4 * a)), dma((2, 4, 2 * a)), dma((2, 4 * a)),
            dma((2, 4 * a)), dma((2, 4 * a)), dma((cores,)), dma((cores,)),
        ],
        compiler_params=pltpu.CompilerParams(
            collective_id=0, has_side_effects=True, vmem_limit_bytes=50 * 1024 * 1024),
    )(block_input, value_cotangent, mixed_output, output_cotangent, value_basis, output_basis, value_weight, output_weight,
      value_mean, value_square, output_mean, output_square)
    return tuple(pl.pallas_call(
        place_out,
        out_shape=[jax.ShapeDtypeStruct(*out) for out in outs],
        in_specs=[vmem] * len(outs),
        out_specs=[hbm] * len(outs),
        scratch_shapes=[dma((len(outs),))],
        compiler_params=pltpu.CompilerParams(vmem_limit_bytes=8 * 1024 * 1024),
    )(*ready))


def solution(mesh):
    placed = (
        P("fs", None),
        P("fs", "tp"),
        P("fs", "tp"),
        P("fs", None),
        P("fs", "tp"),
        P("tp", "fs"),
        P("fs", None),
        P("fs", None),
        P(None, "tp"),
        P(None, "tp"),
        P("tp", None),
        P("tp", None),
    )
    return jax.shard_map(
        on_device,
        mesh=mesh,
        in_specs=placed,
        out_specs=(
            P("fs", "tp"),
            P(None, "tp"),
            P("fs", "tp"),
            P(None, "tp"),
            P(None, "tp"),
            P("tp", "fs"),
            P("tp", None),
            P("tp", "fs"),
            P("tp", None),
            P("tp", None),
        ),
        check_vma=False,
    )
```

```python
import functools
import math

import jax
import jax.numpy as jnp
from jax import lax
from jax.experimental import pallas as pl
from jax.experimental.pallas import tpu as pltpu
from jax.sharding import PartitionSpec as P

MESH = pl.DeviceIdType.MESH
VALUE_RATE = 125.0 / 0.125
OUTPUT_RATE = 125.0 / 0.1875
LOW_RATE = 124.0
BLOCK_LANES = 512
LANES = 128
TOKEN_TILE = 512
FIRST = (((0,), (0,)), ((), ()))
LAST = (((1,), (1,)), ((), ()))


def split_fs(n):
    inner = 2 if n % 2 == 0 else 1
    middle = 2 if n % (2 * inner) == 0 else 1
    return n // (inner * middle), middle, inner


class Place:
    def __init__(self, n):
        self.sizes = split_fs(n)
        self.me = lax.axis_index("fs")
        self.core = lax.axis_index("tp")
        self.par = lax.rem(self.core, 2)
        self.partner = self.core + 1 - 2 * self.par
        a, b, c = self.sizes
        self.z = self.me // (b * c)
        self.y = lax.rem(self.me // c, b)
        self.x = lax.rem(self.me, c)
        self.planes = [self.near(i) for i in range(a)]

    def near(self, i):
        a = self.sizes[0]
        low = jnp.minimum(self.z, a - 1 - self.z)
        side = self.z - (i + 1) // 2 if i % 2 else self.z + i // 2
        return jnp.where(2 * low >= i, side, jnp.where(self.z <= a - 1 - self.z, i, a - 1 - i))

    def on(self, z, ds, dt, par=None):
        a, b, c = self.sizes
        par = self.par if par is None else par
        y = lax.rem(self.y + ds * (1 - par) + dt * par, b)
        x = lax.rem(self.x + ds * par + dt * (1 - par), c)
        return (z * b + y) * c + x

    def at(self, dz, ds, dt):
        return self.on(lax.rem(self.z + dz, self.sizes[0]), ds, dt)


class Gather:
    def __init__(self, place, slot, send, recv, line=False, plane_first=False, seen=None):
        self.p, self.slot, self.send, self.recv = place, slot, send, recv
        self.line, self.plane_first, self.seen = line, plane_first, seen or (lambda *k: None)
        self.a = place.sizes[0]
        self.started = []

    def copy(self, src, ds, to, kind, sid, rid):
        ref = self.slot(self.p.on(src, ds, 0))
        return pltpu.make_async_remote_copy(
            src_ref=ref, dst_ref=ref, send_sem=self.send.at[kind, sid], recv_sem=self.recv.at[rid],
            device_id={"fs": to}, device_id_type=MESH)

    def go(self, src, ds, to, kind, sid, rid, when=None):
        def make():
            return self.copy(src, ds, to, kind, sid, rid)

        self.started.append((make, when))
        if when is None:
            make().start()
        else:
            @pl.when(when)
            def _():
                make().start()

    def came(self, src, ds, dt):
        ref = self.slot(self.p.on(src, ds, dt))
        pltpu.make_async_remote_copy(
            src_ref=ref, dst_ref=ref, send_sem=self.send.at[0, 0], recv_sem=self.recv.at[(src * 2 + ds) * 2 + dt],
            device_id={"fs": self.p.me}, device_id_type=MESH).wait_recv()

    def to_s(self, src):
        self.go(src, 0, self.p.on(self.p.z, 1, 0), 2, src * 2, (src * 2 + 1) * 2)

    def to_t(self, src, ds):
        self.go(src, ds, self.p.on(self.p.z, 0, 1), 3, src * 2 + ds, (src * 2 + ds) * 2 + 1)

    def begin_z(self, ds=0):
        z, rid = self.p.z, (self.p.z * 2 + ds) * 2
        if self.line:
            self.go(z, ds, self.p.on(z + 1, 0, 0), 0, z * 2 + ds, rid, z < self.a - 1)
            self.go(z, ds, self.p.on(z - 1, 0, 0), 1, z * 2 + ds, rid, z > 0)
        else:
            for dz in range(1, self.a):
                self.go(z, ds, self.p.at(dz, 0, 0), 0, dz * 2 + ds, rid)

    def begin_st(self):
        self.to_s(self.p.z)
        self.to_t(self.p.z, 0)
        self.seen(self.p.z, 0, 0)

    def begin(self):
        self.begin_z()
        self.begin_st()

    def near_s(self):
        self.came(self.p.z, 1, 0)
        self.begin_z(1)
        self.to_t(self.p.z, 1)
        self.seen(self.p.z, 1, 0)

    def z(self, k, ds=0):
        if k >= self.a:
            return
        src, z = self.p.planes[k], self.p.z
        self.came(src, ds, 0)
        if self.line:
            up = src < z
            to = jnp.clip(jnp.where(up, z + 1, z - 1), 0, self.a - 1)
            inside = jnp.where(up, z + 1, self.a - z) < self.a
            self.go(src, ds, self.p.on(to, 0, 0), 0, src * 2 + ds, (src * 2 + ds) * 2, inside)
        if not self.plane_first:
            self.to_s(src)
        self.to_t(src, ds)
        self.seen(src, ds, 0)

    def s(self, k):
        if k < self.a:
            src = self.p.planes[k]
            self.came(src, 1, 0)
            self.to_t(src, 1)
            self.seen(src, 1, 0)

    def t(self, k):
        if k < self.a:
            for ds in range(2):
                self.came(self.p.planes[k], ds, 1)
                self.seen(self.p.planes[k], ds, 1)

    def last(self):
        for k in range(self.a):
            self.t(k)

    def finish(self):
        for make, when in self.started:
            if when is None:
                make().wait_send()
            else:
                @pl.when(when)
                def _():
                    make().wait_send()


class Bases(Gather):
    def __init__(self, place, ref, send, recv, c_send, c_recv, plane_first):
        half = ref.shape[1] // 2
        rows = [pl.ds(pl.multiple_of(side * half, half), half) for side in (place.par, 1 - place.par)]
        super().__init__(place, lambda i: ref.at[i, rows[0]], send, recv, line=True, plane_first=plane_first, seen=self.cross)
        self.other = lambda i: ref.at[i, rows[1]]
        self.c_send, self.c_recv = c_send, c_recv
        self.crossed = []

    def over(self, ref, k):
        return pltpu.make_async_remote_copy(
            src_ref=ref, dst_ref=ref, send_sem=self.c_send.at[k], recv_sem=self.c_recv.at[k],
            device_id={"tp": self.p.partner}, device_id_type=MESH)

    def cross(self, src, ds, dt):
        c = self.over(self.slot(self.p.on(src, ds, dt)), (src * 2 + ds) * 2 + dt)
        c.start()
        self.crossed.append(c)

    def whole(self):
        for src in range(self.a):
            for ds in range(2):
                for dt in range(2):
                    self.over(self.other(self.p.on(src, ds, dt, 1 - self.p.par)), (src * 2 + ds) * 2 + dt).wait_recv()

    def finish(self):
        super().finish()
        for c in self.crossed:
            c.wait_send()


def halves(value):
    high = value.astype(jnp.bfloat16)
    return high, (value - high.astype(jnp.float32)).astype(jnp.bfloat16)


def one(reduce, value):
    return reduce(reduce(value, axis=1, keepdims=True), axis=0, keepdims=True)


def bound(values):
    top = jnp.maximum(one(jnp.max, jnp.abs(values)) * 1.01, 1e-30)
    return top.astype(jnp.bfloat16).astype(jnp.float32)


def encode(values, entries, rows):
    high, width = values.shape
    pieces = [jnp.exp2((LOW_RATE / entries[0]) * values[:, at:at + LANES]) for at in range(0, width, LANES)]
    row = lax.broadcasted_iota(jnp.int32, (rows - high * len(pieces), LANES), 0)
    extra = jnp.zeros(row.shape, jnp.float32)
    for k, entry in enumerate(entries):
        extra = jnp.where(row == k, entry.astype(jnp.float32), extra)
    return jnp.concatenate(pieces + [extra], axis=0).astype(jnp.bfloat16)


def decode(code, high, width):
    code = code.astype(jnp.float32)
    end = high * (width // LANES)
    rate = code[end:end + 1] * (1.0 / LOW_RATE)
    pieces = [rate * jnp.log2(code[at:at + high]) for at in range(0, end, high)]
    return jnp.concatenate(pieces, axis=1), code[end:]


class Scatter:
    def __init__(self, place, part, code, got, send, recv):
        self.p, self.part, self.code, self.got, self.send, self.recv = place, part, code, got, send, recv
        self.a = place.sizes[0]
        self.order = list(range(1, self.a)) + [0]
        self.started = []

    def copy(self, block, to, slot):
        return pltpu.make_async_remote_copy(
            src_ref=self.code.at[block], dst_ref=self.got.at[slot],
            send_sem=self.send.at[slot], recv_sem=self.recv.at[slot],
            device_id={"fs": to}, device_id_type=MESH)

    def hand(self, block, to, slot, top):
        self.code[block] = encode(self.part[block], (top,), self.code.shape[1])
        c = self.copy(block, to, slot)
        c.start()
        self.started.append(c)

    def take(self, block, slot):
        self.copy(block, self.p.me, slot).wait_recv()
        value, tail = decode(self.got[slot], *self.part.shape[1:])
        self.part[block] += value
        return tail[:1]

    def grown(self, top):
        return top.astype(jnp.bfloat16).astype(jnp.float32)

    def give_t(self):
        n, high, width = self.part.shape
        self.top = jnp.broadcast_to(bound(self.part[...].reshape(n * high, width)), (1, LANES))
        for dz in self.order:
            for ds in (1, 0):
                self.hand(self.p.at(dz, ds, 1), self.p.on(self.p.z, 0, 1), dz * 2 + ds, self.top)

    def turn_s(self, i):
        if i < self.a:
            dz = self.order[i]
            top = self.take(self.p.at(dz, 1, 0), dz * 2 + 1)
            if i == 0:
                self.top = self.grown(self.top + top)
            self.hand(self.p.at(dz, 1, 0), self.p.on(self.p.z, 1, 0), 2 * self.a + dz, self.top)
            self.take(self.p.at(dz, 0, 0), dz * 2)

    def turn_z(self, i):
        if i < self.a:
            dz = self.order[i]
            top = self.take(self.p.at(dz, 0, 0), 2 * self.a + dz)
            if i == 0:
                self.top = self.grown(self.top + top)
            if dz:
                self.hand(self.p.at(dz, 0, 0), self.p.at(dz, 0, 0), 3 * self.a + dz, self.top)

    def end(self):
        for dz in range(1, self.a):
            self.take(self.p.me, 3 * self.a + dz)

    def finish(self):
        for c in self.started:
            c.wait_send()


def twice(basis):
    return jnp.concatenate([basis, basis], axis=1)


def value_steps(basis, norms):
    return jnp.dot(twice(basis), norms[...], preferred_element_type=jnp.float32)


def output_steps(basis, norms):
    return lax.dot_general(norms[...], twice(basis), LAST, preferred_element_type=jnp.float32)


def copy_plane(place, k, bases, wv, wo, norms_v, norms_o, put_v, put_o):
    depth, rank, width = bases.shape[2], bases.shape[3], wv.shape[2]
    plane = place.sizes[1] * place.sizes[2]
    count = math.gcd(plane, max(1, BLOCK_LANES // depth))
    span = count * depth
    for i in range(plane // count):
        shard = place.planes[k] * plane + i * count
        shards = pl.ds(shard, count)
        at = pl.ds(i * span, span)
        old = jnp.log2(wv[shards].astype(jnp.float32)).reshape(span, width) * (1.0 / VALUE_RATE)
        put_v(at, (old - 0.02 * value_steps(bases[0, shards].reshape(span, rank), norms_v)).astype(jnp.bfloat16))
        old = jnp.concatenate([wo[shard + q].astype(jnp.float32) for q in range(count)], axis=1)
        old = jnp.log2(old) * (1.0 / OUTPUT_RATE)
        put_o(at, (old - 0.02 * output_steps(bases[1, shards].reshape(span, rank), norms_o)).astype(jnp.bfloat16))


def exchange(n, scaling, entries, x_hbm, v_hbm, m_hbm, o_hbm, vb_hbm, ob_hbm, vw_hbm, ow_hbm, vm_hbm, vs_hbm, om_hbm, os_hbm,
             v_copy, vm_next, vs_next, o_copy, om_next, os_next, bases, wv, wo, vw, ow, norms_v, norms_o,
             low, sums, x_ref, v_ref, m_ref, o_ref, vm, vs, om, os, part, code, got, small,
             load_sem, own_sem, b_send, b_recv, c_send, c_recv, w_send, w_recv, l_send, l_recv, r_send, r_recv, q_send, q_recv):
    p = Place(n)
    a, b, c = p.sizes
    par, me = p.par, p.me
    half = bases.shape[2] // 2
    mine = pl.ds(pl.multiple_of(par * half, half), half)
    own = [pltpu.make_async_copy(s.at[mine], bases.at[i, me, mine], own_sem.at[i]) for i, s in enumerate((vb_hbm, ob_hbm))]
    loads = [pltpu.make_async_copy(s, d, load_sem.at[i]) for i, (s, d) in enumerate(
        ((vw_hbm, vw), (ow_hbm, ow), (o_hbm, o_ref), (m_hbm, m_ref), (x_hbm, x_ref), (v_hbm, v_ref),
         (vm_hbm, vm), (vs_hbm, vs), (om_hbm, om), (os_hbm, os)))]
    for c_ in own + loads:
        c_.start()
    barrier = pltpu.get_barrier_semaphore()
    for to, inside in ((p.on(p.z + 1, 0, 0), p.z < a - 1), (p.on(p.z - 1, 0, 0), p.z > 0)):
        @pl.when(inside)
        def _():
            pl.semaphore_signal(barrier, inc=1, device_id={"fs": to}, device_id_type=MESH)

    for to in (p.on(p.z, 1, 0), p.on(p.z, 0, 1)):
        pl.semaphore_signal(barrier, inc=1, device_id={"fs": to}, device_id_type=MESH)
    ends = jnp.where(p.z > 0, 1, 0) + jnp.where(p.z < a - 1, 1, 0)
    cores = lax.axis_size("tp")
    siblings = [lax.rem(p.core + d, cores) for d in range(1, cores)]
    for to in siblings:
        pl.semaphore_signal(barrier, inc=1, device_id={"tp": to}, device_id_type=MESH)
    pl.semaphore_wait(barrier, 2 + len(siblings) + ends)
    for c_ in own:
        c_.wait()

    bv, bo = (Bases(p, bases.at[j], b_send.at[j], b_recv.at[j], c_send.at[j], c_recv.at[j], first)
              for j, first in enumerate((True, False)))
    w0, w1 = (Gather(p, lambda i, ref=ref: ref.at[i], w_send.at[j], w_recv.at[j], line=True, plane_first=first)
              for j, (ref, first) in enumerate(((wv, False), (wo, True))))
    rv, ro = (Scatter(p, part.at[j], code.at[j], got.at[j], r_send.at[j], r_recv.at[j]) for j in range(2))
    lv, lo = (Gather(p, lambda i, j=j: low.at[j, i], l_send.at[j], l_recv.at[j]) for j in range(2))

    depth, rank = bases.shape[2], bases.shape[3]
    high, width = part.shape[2], part.shape[3]
    tokens = x_ref.shape[0]
    tile = math.gcd(tokens, TOKEN_TILE)
    steps = tokens // tile
    far = range(3, a)

    def product(j, start, stop):
        wide, thin = ((x_ref, v_ref), (o_ref, m_ref))[j]

        @pl.loop(start, stop)
        def _(step):
            rows = pl.ds(pl.multiple_of(step * tile, tile), tile)
            thick = jnp.dot(wide[rows, :], bases[j].reshape(n * depth, rank), preferred_element_type=jnp.float32)
            both = jnp.concatenate(halves(thick), axis=0)
            cot = jnp.concatenate([thin[rows, :]] * 2, axis=0)
            part[j] += lax.dot_general(both, cot, FIRST, preferred_element_type=jnp.float32).reshape(n, high, width)

    def pack(j):
        value = part[j, me] * scaling
        low[j, me] = encode(value, (bound(value),) + halves(one(jnp.sum, value * value)), low.shape[2])

    def unpack(j):
        total = jnp.zeros((1, LANES), jnp.float32)
        for i in range(n):
            small[j, i * high:(i + 1) * high], tail = decode(low[j, i], high, width)
            total += tail[1:2] + tail[2:3]
        return total

    def share(total):
        sums[p.core] = jnp.broadcast_to(total, sums.shape[1:])
        out = []
        for d, to in enumerate(siblings):
            out.append(pltpu.make_async_remote_copy(
                src_ref=sums.at[p.core], dst_ref=sums.at[p.core], send_sem=q_send.at[d], recv_sem=q_recv.at[d],
                device_id={"tp": to}, device_id_type=MESH))
            out[-1].start()
        return out

    def shared():
        for d in range(cores - 1):
            ref = sums.at[lax.rem(p.core - d - 1 + cores, cores)]
            pltpu.make_async_remote_copy(
                src_ref=ref, dst_ref=ref, send_sem=q_send.at[d], recv_sem=q_recv.at[d],
                device_id={"tp": p.partner}, device_id_type=MESH).wait_recv()

    def update():
        total = sums[0, :1, :1]
        for i in range(1, cores):
            total += sums[i, :1, :1]
        clip = 1.0 / jnp.sqrt(1.0 + total / entries)
        for scaled, mean, square, mean_next, square_next, norms, at in (
            (clip * small[0], vm, vs, vm_next, vs_next, norms_v, lambda k: (slice(k * rank, (k + 1) * rank), slice(None))),
            (clip * small[1].T, om, os, om_next, os_next, norms_o, lambda k: (slice(None), slice(k * rank, (k + 1) * rank))),
        ):
            mean_new = 0.8 * mean[...] + 0.2 * scaled
            square_new = 0.9 * square[...] + 0.1 * scaled * scaled
            mean_next[...] = mean_new
            square_next[...] = square_new
            for k, part_ in enumerate(halves(mean_new / jnp.sqrt(square_new + 0.1))):
                norms[at(k)] = part_

    def copies(k):
        if k < a:
            span = b * c * depth
            to = pl.ds(pl.multiple_of(p.planes[k] * span, span), span)

            def put_v(at, value):
                v_copy.at[to][at, :] = value

            def put_o(at, value):
                o_copy.at[:, to][:, at] = value

            copy_plane(p, k, bases, wv, wo, norms_v, norms_o, put_v, put_o)

    bv.begin_st()
    bo.begin_st()
    bo.begin_z()
    part[...] = jnp.zeros_like(part)
    for c_ in loads[:2]:
        c_.wait()
    wv[me] = jnp.exp2(VALUE_RATE * vw[...]).astype(wv.dtype)
    wo[me] = jnp.exp2(OUTPUT_RATE * ow[...]).astype(wo.dtype)
    w1.begin_st()
    bv.begin_z()
    bv.near_s()
    bo.z(1)
    bo.z(2)
    bv.z(1)
    bv.z(2)
    bv.z(1, 1)
    bv.z(2, 1)
    for k in far:
        bo.z(k)
    for k in far:
        bv.z(k)
    for k in far:
        bv.z(k, 1)
    w0.begin_z()
    w1.begin_z()
    bo.s(2)
    bo.s(0)
    for k in far:
        bo.s(k)
    bo.s(1)
    w1.near_s()
    bv.last()
    w0.begin_st()
    bv.whole()
    for c_ in loads[4:6]:
        c_.wait()
    product(0, 0, steps // 2)
    bo.last()
    w0.z(1)
    product(0, steps // 2, steps)
    rv.give_t()
    w1.z(1)
    w0.z(2)
    bo.whole()
    for c_ in loads[2:4]:
        c_.wait()
    product(1, 0, steps // 2)
    w1.z(2)
    product(1, steps // 2, steps)
    ro.give_t()
    rv.turn_s(0)
    rv.turn_s(1)
    rv.turn_s(2)
    for k in far:
        w0.z(k)
    for k in far:
        rv.turn_s(k)
    rv.turn_z(0)
    w0.s(0)
    rv.turn_z(1)
    w1.z(1, 1)
    rv.turn_z(2)
    w1.z(2, 1)
    w0.s(2)
    w0.s(1)
    ro.turn_s(0)
    ro.turn_s(1)
    for k in far:
        w1.z(k)
    ro.turn_s(2)
    for k in far:
        ro.turn_s(k)
    ro.turn_z(0)
    for k in far:
        rv.turn_z(k)
    ro.turn_z(1)
    ro.turn_z(2)
    rv.end()
    for k in far:
        w1.z(k, 1)
    w1.t(2)
    for k in far:
        ro.turn_z(k)
    pack(0)
    for k in far:
        w0.s(k)
    lv.begin_z()
    lv.begin_st()
    ro.end()
    pack(1)
    lo.begin_z()
    lv.z(1)
    w1.t(1)
    w1.t(0)
    lv.z(2)
    lo.begin_st()
    for k in far:
        lv.z(k)
    lo.z(1)
    lv.s(0)
    lo.z(2)
    for k in far:
        lo.z(k)
    lo.s(1)
    w0.t(0)
    lv.s(2)
    lv.s(1)
    for k in far:
        lv.s(k)
    lo.s(0)
    for k in far:
        lo.s(k)
    lo.s(2)
    for k in far:
        w0.t(k)
    lv.last()
    total_v = unpack(0)
    lo.last()
    total = unpack(1)
    sent = share(total + total_v)
    for k in far:
        w1.t(k)
    w0.t(2)
    w0.t(1)
    for g in (bo, bv, ro, rv, lo, lv):
        g.finish()
    shared()
    for done in sent:
        done.wait_send()
    for c_ in loads[6:]:
        c_.wait()
    update()
    copies(1)
    copies(0)
    for g in (w0, w1):
        g.finish()


def finish(early, n, v_copy, vm_ready, vs_ready, o_copy, om_ready, os_ready, bases, wv, wo, vw, ow, norms_v, norms_o,
           v_next, v_all, v_step, vm_next, vs_next, o_next, o_all, o_step, om_next, os_next,
           v_new, v_mine, o_new, o_mine, v_late, o_late, sem):
    p = Place(n)
    a, b, c = p.sizes
    span = b * c * bases.shape[2]
    moves = []

    def move(src, dst):
        moves.append(pltpu.make_async_copy(src, dst, sem.at[len(moves)]))
        moves[-1].start()

    def planes(k, v_src, o_src):
        to = pl.ds(pl.multiple_of(p.planes[k] * span, span), span)
        move(v_src(to), v_all.at[to])
        move(o_src(to), o_all.at[:, to])

    for src, dst in ((vm_ready, vm_next), (vs_ready, vs_next), (om_ready, om_next), (os_ready, os_next)):
        move(src, dst)
    for k in range(min(early, a)):
        planes(k, lambda to: v_copy.at[to], lambda to: o_copy.at[:, to])
    for k in range(early, a):
        def put_v(at, value):
            v_late.at[k - early][at, :] = value

        def put_o(at, value):
            o_late.at[k - early][:, at] = value

        copy_plane(p, k, bases, wv, wo, norms_v, norms_o, put_v, put_o)
        planes(k, lambda to: v_late.at[k - early], lambda to: o_late.at[k - early])
    v_mine[...] = value_steps(bases[0, p.me], norms_v)
    v_new[...] = vw[...] - 0.02 * v_mine[...]
    o_mine[...] = output_steps(bases[1, p.me], norms_o)
    o_new[...] = ow[...] - 0.02 * o_mine[...]
    for src, dst in ((v_mine, v_step), (v_new, v_next), (o_mine, o_step), (o_new, o_next)):
        move(src, dst)
    for done in moves:
        done.wait()


def on_device(
    block_input,
    value_cotangent,
    mixed_output,
    output_cotangent,
    value_weight,
    output_weight,
    value_basis,
    output_basis,
    value_mean,
    value_square,
    output_mean,
    output_square,
):
    n, cores = lax.axis_size("fs"), lax.axis_size("tp")
    depth, rank = value_basis.shape
    tokens, width = value_cotangent.shape
    wide = block_input.shape[1]
    a = split_fs(n)[0]
    scaling = 1.0 / math.sqrt(tokens * n)
    entries = 2.0 * rank * width * cores
    f32, b16 = jnp.float32, jnp.bfloat16
    high = rank // n
    rows = (high * (width // LANES) + 10) // 8 * 8
    hbm = pl.BlockSpec(memory_space=pltpu.HBM)
    vmem = pl.BlockSpec(memory_space=pltpu.VMEM)
    dma = pltpu.SemaphoreType.DMA
    v_row, v_all, v_small = ((depth, width), f32), ((n * depth, width), b16), ((rank, width), f32)
    o_row, o_all, o_small = ((width, depth), f32), ((width, n * depth), b16), ((width, rank), f32)
    outs = (v_row, v_all, v_row, v_small, v_small, o_row, o_all, o_row, o_small, o_small)
    early = 2
    span = n // a * depth
    late = max(a - early, 1)
    held = (v_all, v_small, v_small, o_all, o_small, o_small, ((2, n, depth, rank), b16), ((n, depth, width), b16),
            ((n, width, depth), b16), v_row, o_row, ((2 * rank, width), b16), ((width, 2 * rank), b16))
    ready = pl.pallas_call(
        functools.partial(exchange, n, scaling, entries),
        out_shape=[pltpu.VMEM(*out) for out in held],
        in_specs=[hbm] * 12,
        out_specs=[vmem] * len(held),
        scratch_shapes=[
            pltpu.VMEM((2, n, rows, LANES), b16), pltpu.VMEM((cores, 8, LANES), f32),
            pltpu.VMEM((tokens, wide), b16), pltpu.VMEM((tokens, width), b16),
            pltpu.VMEM((tokens, width), b16), pltpu.VMEM((tokens, wide), b16),
            pltpu.VMEM((rank, width), f32), pltpu.VMEM((rank, width), f32),
            pltpu.VMEM((width, rank), f32), pltpu.VMEM((width, rank), f32),
            pltpu.VMEM((2, n, high, width), f32), pltpu.VMEM((2, n, rows, LANES), b16), pltpu.VMEM((2, 4 * a, rows, LANES), b16),
            pltpu.VMEM((2, rank, width), f32),
            dma((10,)), dma((2,)),
            dma((2, 4, 2 * a)), dma((2, 4 * a)), dma((2, 4 * a)), dma((2, 4 * a)),
            dma((2, 4, 2 * a)), dma((2, 4 * a)), dma((2, 4, 2 * a)), dma((2, 4 * a)),
            dma((2, 4 * a)), dma((2, 4 * a)), dma((cores,)), dma((cores,)),
        ],
        compiler_params=pltpu.CompilerParams(
            collective_id=0, has_side_effects=True, vmem_limit_bytes=40 * 1024 * 1024),
    )(block_input, value_cotangent, mixed_output, output_cotangent, value_basis, output_basis, value_weight, output_weight,
      value_mean, value_square, output_mean, output_square)
    return tuple(pl.pallas_call(
        functools.partial(finish, early, n),
        out_shape=[jax.ShapeDtypeStruct(*out) for out in outs],
        in_specs=[vmem] * len(held),
        out_specs=[hbm] * len(outs),
        scratch_shapes=[
            pltpu.VMEM(*v_row), pltpu.VMEM(*v_row), pltpu.VMEM(*o_row), pltpu.VMEM(*o_row),
            pltpu.VMEM((late, span, width), b16), pltpu.VMEM((late, width, span), b16), dma((8 + 2 * a,))],
        compiler_params=pltpu.CompilerParams(vmem_limit_bytes=16 * 1024 * 1024),
    )(*ready))


def solution(mesh):
    placed = (
        P("fs", None),
        P("fs", "tp"),
        P("fs", "tp"),
        P("fs", None),
        P("fs", "tp"),
        P("tp", "fs"),
        P("fs", None),
        P("fs", None),
        P(None, "tp"),
        P(None, "tp"),
        P("tp", None),
        P("tp", None),
    )
    return jax.shard_map(
        on_device,
        mesh=mesh,
        in_specs=placed,
        out_specs=(
            P("fs", "tp"),
            P(None, "tp"),
            P("fs", "tp"),
            P(None, "tp"),
            P(None, "tp"),
            P("tp", "fs"),
            P("tp", None),
            P("tp", "fs"),
            P("tp", None),
            P("tp", None),
        ),
        check_vma=False,
    )
```

```python
import functools
import math

import jax
import jax.numpy as jnp
from jax import lax
from jax.experimental import pallas as pl
from jax.experimental.pallas import tpu as pltpu
from jax.sharding import PartitionSpec as P

MESH = pl.DeviceIdType.MESH
VALUE_RATE = 125.0 / 0.125
OUTPUT_RATE = 125.0 / 0.1875
LOW_RATE = 124.0
BLOCK_LANES = 512
LANES = 128
TOKEN_TILE = 512
FIRST = (((0,), (0,)), ((), ()))
LAST = (((1,), (1,)), ((), ()))


def split_fs(n):
    inner = 2 if n % 2 == 0 else 1
    middle = 2 if n % (2 * inner) == 0 else 1
    return n // (inner * middle), middle, inner


class Place:
    def __init__(self, n):
        self.sizes = split_fs(n)
        self.me = lax.axis_index("fs")
        self.core = lax.axis_index("tp")
        self.par = lax.rem(self.core, 2)
        self.partner = self.core + 1 - 2 * self.par
        a, b, c = self.sizes
        self.z = self.me // (b * c)
        self.y = lax.rem(self.me // c, b)
        self.x = lax.rem(self.me, c)
        self.planes = [self.near(i) for i in range(a)]

    def near(self, i):
        a = self.sizes[0]
        low = jnp.minimum(self.z, a - 1 - self.z)
        side = self.z - (i + 1) // 2 if i % 2 else self.z + i // 2
        return jnp.where(2 * low >= i, side, jnp.where(self.z <= a - 1 - self.z, i, a - 1 - i))

    def on(self, z, ds, dt, par=None):
        a, b, c = self.sizes
        par = self.par if par is None else par
        y = lax.rem(self.y + ds * (1 - par) + dt * par, b)
        x = lax.rem(self.x + ds * par + dt * (1 - par), c)
        return (z * b + y) * c + x

    def at(self, dz, ds, dt):
        return self.on(lax.rem(self.z + dz, self.sizes[0]), ds, dt)


class Gather:
    def __init__(self, place, slot, send, recv, line=False, plane_first=False, seen=None):
        self.p, self.slot, self.send, self.recv = place, slot, send, recv
        self.line, self.plane_first, self.seen = line, plane_first, seen or (lambda *k: None)
        self.a = place.sizes[0]
        self.started = []

    def copy(self, src, ds, to, kind, sid, rid):
        ref = self.slot(self.p.on(src, ds, 0))
        return pltpu.make_async_remote_copy(
            src_ref=ref, dst_ref=ref, send_sem=self.send.at[kind, sid], recv_sem=self.recv.at[rid],
            device_id={"fs": to}, device_id_type=MESH)

    def go(self, src, ds, to, kind, sid, rid, when=None):
        def make():
            return self.copy(src, ds, to, kind, sid, rid)

        self.started.append((make, when))
        if when is None:
            make().start()
        else:
            @pl.when(when)
            def _():
                make().start()

    def came(self, src, ds, dt):
        ref = self.slot(self.p.on(src, ds, dt))
        pltpu.make_async_remote_copy(
            src_ref=ref, dst_ref=ref, send_sem=self.send.at[0, 0], recv_sem=self.recv.at[(src * 2 + ds) * 2 + dt],
            device_id={"fs": self.p.me}, device_id_type=MESH).wait_recv()

    def to_s(self, src):
        self.go(src, 0, self.p.on(self.p.z, 1, 0), 2, src * 2, (src * 2 + 1) * 2)

    def to_t(self, src, ds):
        self.go(src, ds, self.p.on(self.p.z, 0, 1), 3, src * 2 + ds, (src * 2 + ds) * 2 + 1)

    def begin_z(self, ds=0):
        z, rid = self.p.z, (self.p.z * 2 + ds) * 2
        if self.line:
            self.go(z, ds, self.p.on(z + 1, 0, 0), 0, z * 2 + ds, rid, z < self.a - 1)
            self.go(z, ds, self.p.on(z - 1, 0, 0), 1, z * 2 + ds, rid, z > 0)
        else:
            for dz in range(1, self.a):
                self.go(z, ds, self.p.at(dz, 0, 0), 0, dz * 2 + ds, rid)

    def begin_st(self):
        self.to_s(self.p.z)
        self.to_t(self.p.z, 0)
        self.seen(self.p.z, 0, 0)

    def begin(self):
        self.begin_z()
        self.begin_st()

    def near_s(self):
        self.came(self.p.z, 1, 0)
        self.begin_z(1)
        self.to_t(self.p.z, 1)
        self.seen(self.p.z, 1, 0)

    def z(self, k, ds=0):
        if k >= self.a:
            return
        src, z = self.p.planes[k], self.p.z
        self.came(src, ds, 0)
        if self.line:
            up = src < z
            to = jnp.clip(jnp.where(up, z + 1, z - 1), 0, self.a - 1)
            inside = jnp.where(up, z + 1, self.a - z) < self.a
            self.go(src, ds, self.p.on(to, 0, 0), 0, src * 2 + ds, (src * 2 + ds) * 2, inside)
        if not self.plane_first:
            self.to_s(src)
        self.to_t(src, ds)
        self.seen(src, ds, 0)

    def s(self, k):
        if k < self.a:
            src = self.p.planes[k]
            self.came(src, 1, 0)
            self.to_t(src, 1)
            self.seen(src, 1, 0)

    def t(self, k):
        if k < self.a:
            for ds in range(2):
                self.came(self.p.planes[k], ds, 1)
                self.seen(self.p.planes[k], ds, 1)

    def last(self):
        for k in range(self.a):
            self.t(k)

    def finish(self):
        for make, when in self.started:
            if when is None:
                make().wait_send()
            else:
                @pl.when(when)
                def _():
                    make().wait_send()


class Bases(Gather):
    def __init__(self, place, ref, send, recv, c_send, c_recv, plane_first):
        half = ref.shape[1] // 2
        rows = [pl.ds(pl.multiple_of(side * half, half), half) for side in (place.par, 1 - place.par)]
        super().__init__(place, lambda i: ref.at[i, rows[0]], send, recv, line=True, plane_first=plane_first, seen=self.cross)
        self.other = lambda i: ref.at[i, rows[1]]
        self.c_send, self.c_recv = c_send, c_recv
        self.crossed = []

    def over(self, ref, k):
        return pltpu.make_async_remote_copy(
            src_ref=ref, dst_ref=ref, send_sem=self.c_send.at[k], recv_sem=self.c_recv.at[k],
            device_id={"tp": self.p.partner}, device_id_type=MESH)

    def cross(self, src, ds, dt):
        c = self.over(self.slot(self.p.on(src, ds, dt)), (src * 2 + ds) * 2 + dt)
        c.start()
        self.crossed.append(c)

    def whole(self):
        for src in range(self.a):
            for ds in range(2):
                for dt in range(2):
                    self.over(self.other(self.p.on(src, ds, dt, 1 - self.p.par)), (src * 2 + ds) * 2 + dt).wait_recv()

    def finish(self):
        super().finish()
        for c in self.crossed:
            c.wait_send()


def halves(value):
    high = value.astype(jnp.bfloat16)
    return high, (value - high.astype(jnp.float32)).astype(jnp.bfloat16)


def one(reduce, value):
    return reduce(reduce(value, axis=1, keepdims=True), axis=0, keepdims=True)


def bound(values):
    top = jnp.maximum(one(jnp.max, jnp.abs(values)) * 1.01, 1e-30)
    return top.astype(jnp.bfloat16).astype(jnp.float32)


def encode(values, entries, rows):
    high, width = values.shape
    pieces = [jnp.exp2((LOW_RATE / entries[0]) * values[:, at:at + LANES]) for at in range(0, width, LANES)]
    row = lax.broadcasted_iota(jnp.int32, (rows - high * len(pieces), LANES), 0)
    extra = jnp.zeros(row.shape, jnp.float32)
    for k, entry in enumerate(entries):
        extra = jnp.where(row == k, entry.astype(jnp.float32), extra)
    return jnp.concatenate(pieces + [extra], axis=0).astype(jnp.bfloat16)


def decode(code, high, width):
    code = code.astype(jnp.float32)
    end = high * (width // LANES)
    rate = code[end:end + 1] * (1.0 / LOW_RATE)
    pieces = [rate * jnp.log2(code[at:at + high]) for at in range(0, end, high)]
    return jnp.concatenate(pieces, axis=1), code[end:]


class Scatter:
    def __init__(self, place, part, code, got, send, recv):
        self.p, self.part, self.code, self.got, self.send, self.recv = place, part, code, got, send, recv
        self.a = place.sizes[0]
        self.order = list(range(1, self.a)) + [0]
        self.started = []

    def copy(self, block, to, slot):
        return pltpu.make_async_remote_copy(
            src_ref=self.code.at[block], dst_ref=self.got.at[slot],
            send_sem=self.send.at[slot], recv_sem=self.recv.at[slot],
            device_id={"fs": to}, device_id_type=MESH)

    def hand(self, block, to, slot, top):
        self.code[block] = encode(self.part[block], (top,), self.code.shape[1])
        c = self.copy(block, to, slot)
        c.start()
        self.started.append(c)

    def take(self, block, slot):
        self.copy(block, self.p.me, slot).wait_recv()
        value, tail = decode(self.got[slot], *self.part.shape[1:])
        self.part[block] += value
        return tail[:1]

    def grown(self, top):
        return top.astype(jnp.bfloat16).astype(jnp.float32)

    def give_t(self):
        n, high, width = self.part.shape
        self.top = jnp.broadcast_to(bound(self.part[...].reshape(n * high, width)), (1, LANES))
        for dz in self.order:
            for ds in (1, 0):
                self.hand(self.p.at(dz, ds, 1), self.p.on(self.p.z, 0, 1), dz * 2 + ds, self.top)

    def turn_s(self, i):
        if i < self.a:
            dz = self.order[i]
            top = self.take(self.p.at(dz, 1, 0), dz * 2 + 1)
            if i == 0:
                self.top = self.grown(self.top + top)
            self.hand(self.p.at(dz, 1, 0), self.p.on(self.p.z, 1, 0), 2 * self.a + dz, self.top)
            self.take(self.p.at(dz, 0, 0), dz * 2)

    def turn_z(self, i):
        if i < self.a:
            dz = self.order[i]
            top = self.take(self.p.at(dz, 0, 0), 2 * self.a + dz)
            if i == 0:
                self.top = self.grown(self.top + top)
            if dz:
                self.hand(self.p.at(dz, 0, 0), self.p.at(dz, 0, 0), 3 * self.a + dz, self.top)

    def end(self):
        for dz in range(1, self.a):
            self.take(self.p.me, 3 * self.a + dz)

    def finish(self):
        for c in self.started:
            c.wait_send()


def twice(basis):
    return jnp.concatenate([basis, basis], axis=1)


def value_steps(basis, norms):
    return jnp.dot(twice(basis), norms[...], preferred_element_type=jnp.float32)


def output_steps(basis, norms):
    return lax.dot_general(norms[...], twice(basis), LAST, preferred_element_type=jnp.float32)


def copy_plane(place, k, bases, wv, wo, norms_v, norms_o, put_v, put_o):
    depth, rank, width = bases.shape[2], bases.shape[3], wv.shape[2]
    plane = place.sizes[1] * place.sizes[2]
    count = math.gcd(plane, max(1, BLOCK_LANES // depth))
    span = count * depth
    for i in range(plane // count):
        shard = place.planes[k] * plane + i * count
        shards = pl.ds(shard, count)
        at = pl.ds(i * span, span)
        old = jnp.log2(wv[shards].astype(jnp.float32)).reshape(span, width) * (1.0 / VALUE_RATE)
        put_v(at, (old - 0.02 * value_steps(bases[0, shards].reshape(span, rank), norms_v)).astype(jnp.bfloat16))
        old = jnp.concatenate([wo[shard + q].astype(jnp.float32) for q in range(count)], axis=1)
        old = jnp.log2(old) * (1.0 / OUTPUT_RATE)
        put_o(at, (old - 0.02 * output_steps(bases[1, shards].reshape(span, rank), norms_o)).astype(jnp.bfloat16))


def exchange(n, scaling, entries, x_hbm, v_hbm, m_hbm, o_hbm, vb_hbm, ob_hbm, vw_hbm, ow_hbm, vm_hbm, vs_hbm, om_hbm, os_hbm,
             v_copy, vm_next, vs_next, o_copy, om_next, os_next, bases, wv, wo, vw, ow, norms_v, norms_o,
             low, sums, x_ref, v_ref, m_ref, o_ref, vm, vs, om, os, part, code, got, small,
             load_sem, own_sem, b_send, b_recv, c_send, c_recv, w_send, w_recv, l_send, l_recv, r_send, r_recv, q_send, q_recv):
    p = Place(n)
    a, b, c = p.sizes
    par, me = p.par, p.me
    half = bases.shape[2] // 2
    mine = pl.ds(pl.multiple_of(par * half, half), half)
    own = [pltpu.make_async_copy(s.at[mine], bases.at[i, me, mine], own_sem.at[i]) for i, s in enumerate((vb_hbm, ob_hbm))]
    loads = [pltpu.make_async_copy(s, d, load_sem.at[i]) for i, (s, d) in enumerate(
        ((vw_hbm, vw), (ow_hbm, ow), (o_hbm, o_ref), (m_hbm, m_ref), (x_hbm, x_ref), (v_hbm, v_ref),
         (vm_hbm, vm), (vs_hbm, vs), (om_hbm, om), (os_hbm, os)))]
    for c_ in own + loads:
        c_.start()
    barrier = pltpu.get_barrier_semaphore()
    for to, inside in ((p.on(p.z + 1, 0, 0), p.z < a - 1), (p.on(p.z - 1, 0, 0), p.z > 0)):
        @pl.when(inside)
        def _():
            pl.semaphore_signal(barrier, inc=1, device_id={"fs": to}, device_id_type=MESH)

    for to in (p.on(p.z, 1, 0), p.on(p.z, 0, 1)):
        pl.semaphore_signal(barrier, inc=1, device_id={"fs": to}, device_id_type=MESH)
    ends = jnp.where(p.z > 0, 1, 0) + jnp.where(p.z < a - 1, 1, 0)
    cores = lax.axis_size("tp")
    siblings = [lax.rem(p.core + d, cores) for d in range(1, cores)]
    for to in siblings:
        pl.semaphore_signal(barrier, inc=1, device_id={"tp": to}, device_id_type=MESH)
    pl.semaphore_wait(barrier, 2 + len(siblings) + ends)
    for c_ in own:
        c_.wait()

    bv, bo = (Bases(p, bases.at[j], b_send.at[j], b_recv.at[j], c_send.at[j], c_recv.at[j], first)
              for j, first in enumerate((True, False)))
    w0, w1 = (Gather(p, lambda i, ref=ref: ref.at[i], w_send.at[j], w_recv.at[j], line=True, plane_first=first)
              for j, (ref, first) in enumerate(((wv, False), (wo, True))))
    rv, ro = (Scatter(p, part.at[j], code.at[j], got.at[j], r_send.at[j], r_recv.at[j]) for j in range(2))
    lv, lo = (Gather(p, lambda i, j=j: low.at[j, i], l_send.at[j], l_recv.at[j]) for j in range(2))

    depth, rank = bases.shape[2], bases.shape[3]
    high, width = part.shape[2], part.shape[3]
    tokens = x_ref.shape[0]
    tile = math.gcd(tokens, TOKEN_TILE)
    steps = tokens // tile
    far = range(3, a)

    def product(j, start, stop):
        wide, thin = ((x_ref, v_ref), (o_ref, m_ref))[j]

        @pl.loop(start, stop)
        def _(step):
            rows = pl.ds(pl.multiple_of(step * tile, tile), tile)
            thick = jnp.dot(wide[rows, :], bases[j].reshape(n * depth, rank), preferred_element_type=jnp.float32)
            both = jnp.concatenate(halves(thick), axis=0)
            cot = jnp.concatenate([thin[rows, :]] * 2, axis=0)
            part[j] += lax.dot_general(both, cot, FIRST, preferred_element_type=jnp.float32).reshape(n, high, width)

    def pack(j):
        value = part[j, me] * scaling
        low[j, me] = encode(value, (bound(value),) + halves(one(jnp.sum, value * value)), low.shape[2])

    def unpack(j):
        total = jnp.zeros((1, LANES), jnp.float32)
        for i in range(n):
            small[j, i * high:(i + 1) * high], tail = decode(low[j, i], high, width)
            total += tail[1:2] + tail[2:3]
        return total

    def share(total):
        sums[p.core] = jnp.broadcast_to(total, sums.shape[1:])
        out = []
        for d, to in enumerate(siblings):
            out.append(pltpu.make_async_remote_copy(
                src_ref=sums.at[p.core], dst_ref=sums.at[p.core], send_sem=q_send.at[d], recv_sem=q_recv.at[d],
                device_id={"tp": to}, device_id_type=MESH))
            out[-1].start()
        return out

    def shared():
        for d in range(cores - 1):
            ref = sums.at[lax.rem(p.core - d - 1 + cores, cores)]
            pltpu.make_async_remote_copy(
                src_ref=ref, dst_ref=ref, send_sem=q_send.at[d], recv_sem=q_recv.at[d],
                device_id={"tp": p.partner}, device_id_type=MESH).wait_recv()

    def update():
        total = sums[0, :1, :1]
        for i in range(1, cores):
            total += sums[i, :1, :1]
        clip = 1.0 / jnp.sqrt(1.0 + total / entries)
        for scaled, mean, square, mean_next, square_next, norms, at in (
            (clip * small[0], vm, vs, vm_next, vs_next, norms_v, lambda k: (slice(k * rank, (k + 1) * rank), slice(None))),
            (clip * small[1].T, om, os, om_next, os_next, norms_o, lambda k: (slice(None), slice(k * rank, (k + 1) * rank))),
        ):
            mean_new = 0.8 * mean[...] + 0.2 * scaled
            square_new = 0.9 * square[...] + 0.1 * scaled * scaled
            mean_next[...] = mean_new
            square_next[...] = square_new
            for k, part_ in enumerate(halves(mean_new / jnp.sqrt(square_new + 0.1))):
                norms[at(k)] = part_

    def copies(k):
        if k < a:
            span = b * c * depth
            to = pl.ds(pl.multiple_of(p.planes[k] * span, span), span)

            def put_v(at, value):
                v_copy.at[to][at, :] = value

            def put_o(at, value):
                o_copy.at[:, to][:, at] = value

            copy_plane(p, k, bases, wv, wo, norms_v, norms_o, put_v, put_o)

    bo.begin_st()
    bo.begin_z()
    bv.begin_z()
    bv.begin_st()
    part[...] = jnp.zeros_like(part)
    for c_ in loads[:2]:
        c_.wait()
    wv[me] = jnp.exp2(VALUE_RATE * vw[...]).astype(wv.dtype)
    wo[me] = jnp.exp2(OUTPUT_RATE * ow[...]).astype(wo.dtype)
    w1.begin_z()
    w0.begin_st()
    bo.z(1)
    bv.near_s()
    bv.z(1)
    bo.z(2)
    w1.begin_st()
    w0.begin_z()
    bv.z(2)
    bo.s(0)
    bv.z(2, 1)
    bo.s(2)
    for k in far:
        bo.z(k)
    bo.s(1)
    bv.z(1, 1)
    for k in far:
        bo.s(k)
    for k in far:
        bv.z(k)
    for k in far:
        bv.z(k, 1)
    w1.z(1)
    w1.z(2)
    w1.near_s()
    bo.last()
    w0.z(1)
    bv.last()
    bo.whole()
    for c_ in loads[2:4]:
        c_.wait()
    product(1, 0, steps // 2)
    product(1, steps // 2, steps)
    bv.whole()
    w0.z(2)
    ro.give_t()
    for c_ in loads[4:6]:
        c_.wait()
    product(0, 0, steps // 2)
    product(0, steps // 2, steps)
    rv.give_t()
    w1.z(2, 1)
    w1.z(1, 1)
    w0.s(0)
    ro.turn_s(0)
    ro.turn_s(1)
    ro.turn_s(2)
    for k in far:
        w1.z(k)
    for k in far:
        ro.turn_s(k)
    ro.turn_z(0)
    rv.turn_s(0)
    rv.turn_s(1)
    ro.turn_z(1)
    ro.turn_z(2)
    rv.turn_s(2)
    for k in far:
        w0.z(k)
    for k in far:
        rv.turn_s(k)
    rv.turn_z(0)
    rv.turn_z(1)
    rv.turn_z(2)
    for k in far:
        ro.turn_z(k)
    for k in far:
        w1.z(k, 1)
    ro.end()
    pack(1)
    lo.begin_z()
    for k in far:
        rv.turn_z(k)
    for k in far:
        w0.s(k)
    rv.end()
    pack(0)
    lv.begin_z()
    lo.begin_st()
    lv.begin_st()
    lo.z(1)
    lv.z(1)
    for k in far:
        lo.z(k)
    w1.t(0)
    lo.z(2)
    lo.s(0)
    lv.z(2)
    for k in far:
        lv.z(k)
    lo.s(1)
    for k in far:
        lo.s(k)
    lo.s(2)
    lv.s(1)
    lv.s(2)
    lv.s(0)
    for k in far:
        lv.s(k)
    w0.s(2)
    w0.s(1)
    w1.t(1)
    w1.t(2)
    lo.last()
    w0.t(0)
    for k in far:
        w1.t(k)
    total = unpack(1)
    for k in far:
        w0.t(k)
    lv.last()
    total_v = unpack(0)
    sent = share(total + total_v)
    w0.t(2)
    for g in (bo, bv, ro, rv, lo, lv):
        g.finish()
    shared()
    for done in sent:
        done.wait_send()
    for c_ in loads[6:]:
        c_.wait()
    update()
    w0.t(1)
    for g in (w0, w1):
        g.finish()


def finish(early, n, v_copy, vm_ready, vs_ready, o_copy, om_ready, os_ready, bases, wv, wo, vw, ow, norms_v, norms_o,
           v_next, v_all, v_step, vm_next, vs_next, o_next, o_all, o_step, om_next, os_next,
           v_new, v_mine, o_new, o_mine, v_late, o_late, sem):
    p = Place(n)
    a, b, c = p.sizes
    span = b * c * bases.shape[2]
    moves = []

    def move(src, dst):
        moves.append(pltpu.make_async_copy(src, dst, sem.at[len(moves)]))
        moves[-1].start()

    def planes(k, v_src, o_src):
        to = pl.ds(pl.multiple_of(p.planes[k] * span, span), span)
        move(v_src(to), v_all.at[to])
        move(o_src(to), o_all.at[:, to])

    for src, dst in ((vm_ready, vm_next), (vs_ready, vs_next), (om_ready, om_next), (os_ready, os_next)):
        move(src, dst)
    for k in range(min(early, a)):
        planes(k, lambda to: v_copy.at[to], lambda to: o_copy.at[:, to])
    for k in range(early, a):
        def put_v(at, value):
            v_late.at[k - early][at, :] = value

        def put_o(at, value):
            o_late.at[k - early][:, at] = value

        copy_plane(p, k, bases, wv, wo, norms_v, norms_o, put_v, put_o)
        planes(k, lambda to: v_late.at[k - early], lambda to: o_late.at[k - early])
    v_mine[...] = value_steps(bases[0, p.me], norms_v)
    v_new[...] = vw[...] - 0.02 * v_mine[...]
    o_mine[...] = output_steps(bases[1, p.me], norms_o)
    o_new[...] = ow[...] - 0.02 * o_mine[...]
    for src, dst in ((v_mine, v_step), (v_new, v_next), (o_mine, o_step), (o_new, o_next)):
        move(src, dst)
    for done in moves:
        done.wait()


def on_device(
    block_input,
    value_cotangent,
    mixed_output,
    output_cotangent,
    value_weight,
    output_weight,
    value_basis,
    output_basis,
    value_mean,
    value_square,
    output_mean,
    output_square,
):
    n, cores = lax.axis_size("fs"), lax.axis_size("tp")
    depth, rank = value_basis.shape
    tokens, width = value_cotangent.shape
    wide = block_input.shape[1]
    a = split_fs(n)[0]
    scaling = 1.0 / math.sqrt(tokens * n)
    entries = 2.0 * rank * width * cores
    f32, b16 = jnp.float32, jnp.bfloat16
    high = rank // n
    rows = (high * (width // LANES) + 10) // 8 * 8
    hbm = pl.BlockSpec(memory_space=pltpu.HBM)
    vmem = pl.BlockSpec(memory_space=pltpu.VMEM)
    dma = pltpu.SemaphoreType.DMA
    v_row, v_all, v_small = ((depth, width), f32), ((n * depth, width), b16), ((rank, width), f32)
    o_row, o_all, o_small = ((width, depth), f32), ((width, n * depth), b16), ((width, rank), f32)
    outs = (v_row, v_all, v_row, v_small, v_small, o_row, o_all, o_row, o_small, o_small)
    early = 0
    span = n // a * depth
    late = max(a - early, 1)
    held = (v_all, v_small, v_small, o_all, o_small, o_small, ((2, n, depth, rank), b16), ((n, depth, width), b16),
            ((n, width, depth), b16), v_row, o_row, ((2 * rank, width), b16), ((width, 2 * rank), b16))
    ready = pl.pallas_call(
        functools.partial(exchange, n, scaling, entries),
        out_shape=[pltpu.VMEM(*out) for out in held],
        in_specs=[hbm] * 12,
        out_specs=[vmem] * len(held),
        scratch_shapes=[
            pltpu.VMEM((2, n, rows, LANES), b16), pltpu.VMEM((cores, 8, LANES), f32),
            pltpu.VMEM((tokens, wide), b16), pltpu.VMEM((tokens, width), b16),
            pltpu.VMEM((tokens, width), b16), pltpu.VMEM((tokens, wide), b16),
            pltpu.VMEM((rank, width), f32), pltpu.VMEM((rank, width), f32),
            pltpu.VMEM((width, rank), f32), pltpu.VMEM((width, rank), f32),
            pltpu.VMEM((2, n, high, width), f32), pltpu.VMEM((2, n, rows, LANES), b16), pltpu.VMEM((2, 4 * a, rows, LANES), b16),
            pltpu.VMEM((2, rank, width), f32),
            dma((10,)), dma((2,)),
            dma((2, 4, 2 * a)), dma((2, 4 * a)), dma((2, 4 * a)), dma((2, 4 * a)),
            dma((2, 4, 2 * a)), dma((2, 4 * a)), dma((2, 4, 2 * a)), dma((2, 4 * a)),
            dma((2, 4 * a)), dma((2, 4 * a)), dma((cores,)), dma((cores,)),
        ],
        compiler_params=pltpu.CompilerParams(
            collective_id=0, has_side_effects=True, vmem_limit_bytes=40 * 1024 * 1024),
    )(block_input, value_cotangent, mixed_output, output_cotangent, value_basis, output_basis, value_weight, output_weight,
      value_mean, value_square, output_mean, output_square)
    return tuple(pl.pallas_call(
        functools.partial(finish, early, n),
        out_shape=[jax.ShapeDtypeStruct(*out) for out in outs],
        in_specs=[vmem] * len(held),
        out_specs=[hbm] * len(outs),
        scratch_shapes=[
            pltpu.VMEM(*v_row), pltpu.VMEM(*v_row), pltpu.VMEM(*o_row), pltpu.VMEM(*o_row),
            pltpu.VMEM((late, span, width), b16), pltpu.VMEM((late, width, span), b16), dma((8 + 2 * a,))],
        compiler_params=pltpu.CompilerParams(vmem_limit_bytes=16 * 1024 * 1024),
    )(*ready))


def solution(mesh):
    placed = (
        P("fs", None),
        P("fs", "tp"),
        P("fs", "tp"),
        P("fs", None),
        P("fs", "tp"),
        P("tp", "fs"),
        P("fs", None),
        P("fs", None),
        P(None, "tp"),
        P(None, "tp"),
        P("tp", None),
        P("tp", None),
    )
    return jax.shard_map(
        on_device,
        mesh=mesh,
        in_specs=placed,
        out_specs=(
            P("fs", "tp"),
            P(None, "tp"),
            P("fs", "tp"),
            P(None, "tp"),
            P(None, "tp"),
            P("tp", "fs"),
            P("tp", None),
            P("tp", "fs"),
            P("tp", None),
            P("tp", None),
        ),
        check_vma=False,
    )
```
